32 devices in a mesh: fs: 8 (over z, y), tp: 4 (over x, core).
Axes of the slice: x: 2, y: 2, z: 4, core: 2. Of those that a mesh axis runs over, the one named last changes fastest.
Arguments:
- tokens: bfloat16 [4096, 2048], P(('fs', 'tp')), may hold values from -6 to 6
- pool_in: float32 [2048, 2048], P('fs'), may hold values from -0.125 to 0.125
- pool_mix: float32 [512, 2048], P(None, 'tp'), may hold values from -0.25 to 0.25
- pool_out: float32 [2048, 2048], P('tp', 'fs'), may hold values from -0.125 to 0.125
- ffn_value: float32 [2048, 5632], P('fs', 'tp'), may hold values from -0.125 to 0.125
- ffn_gate: float32 [2048, 5632], P('fs', 'tp'), may hold values from -0.125 to 0.125
- ffn_down: float32 [5632, 2048], P('tp', 'fs'), may hold values from -0.078125 to 0.078125
- conv_weight: float32 [3, 5632], P(None, 'tp'), may hold values from -3.5 to 3.5
- conv_bias: float32 [5632], P('tp'), may hold values from -3 to 3
- pool_in_scale: float32 [2048], replicated, may hold values from 0.5 to 2
- pool_mix_scale: float32 [2048], P('tp'), may hold values from 0.5 to 2
- pool_out_scale: float32 [2048], P('fs'), may hold values from 0.5 to 2
- value_scale: float32 [5632], P('tp'), may hold values from 0.5 to 2
- gate_scale: float32 [5632], P('tp'), may hold values from 0.5 to 2
- down_scale: float32 [2048], P('fs'), may hold values from 0.5 to 2
- norm1_gain: float32 [2048], replicated, may hold values from 0.1 to 1.9
- norm1_bias: float32 [2048], replicated, may hold values from -3 to 3
- norm2_gain: float32 [2048], replicated, may hold values from 0.1 to 1.9
- norm2_bias: float32 [2048], replicated, may hold values from -3 to 3
Outputs:
- layer_out: bfloat16 [4096, 2048], P(('fs', 'tp'))
The draws below stay inside these ranges and needn't reach their ends.
All inputs are finite; a program needn't handle non-finite values.
Results may differ from the reference program's by a relative error of at most 0.015.
Values may be sent and summed in bfloat16 or wider, within the bound.
No kernel may reach another device: no remote copies, remote signals or barrier semaphores. Data moves between devices by JAX's collectives and lax.ppermute only.
A program may use at most 64 MiB of HBM per device.

```python
import math
import jax
import jax.numpy as jnp
from jax import lax

D = 2048
D_POOL = 2048
FF = 5632
GRID = 64
TOK_DEV = 128
GROUP = 512
TOKENS = 4096
N_FS = 8
N_TP = 4


def block_levels(key, dims, shards, low, high):
    factor_of, own = 1.0, jax.random.fold_in(key, 6)
    for position, parts in shards:
        draws = jnp.exp(jax.random.uniform(jax.random.fold_in(own, position), (parts,), jnp.float32, low / len(shards), high / len(shards)))
        factor_of = factor_of * jnp.repeat(draws, dims[position] // parts).reshape([-1 if axis == position else 1 for axis in range(len(dims))])
    return factor_of


def centred(own_key, shape, scale, most, cuts=(), dtype=jnp.bfloat16):
    array = jax.random.normal(own_key, shape, jnp.float32) * scale
    if len(cuts) > 0:
        array = block_levels(own_key, shape, cuts, -0.22, 0.18) * array
    return jnp.clip(array, min=-most, max=most).astype(dtype)


def setup_inputs(seed: int = 0) -> dict:
    seeds = jax.random.split(jax.random.key(seed), 20)
    return {
        "tokens": centred(seeds[0], (TOKENS, D), 1.0, 6.0, ((0, 32),)),
        "pool_in": centred(seeds[1], (D, D_POOL), D ** -0.5, 0.125, ((0, 8),), jnp.float32),
        "pool_mix": centred(seeds[2], (GROUP, D_POOL), GROUP ** -0.5, 0.25, ((1, 4),), jnp.float32),
        "pool_out": centred(seeds[3], (D_POOL, D), D_POOL ** -0.5, 0.125, ((0, 4), (1, 8)), jnp.float32),
        "ffn_value": centred(seeds[4], (D, FF), D ** -0.5, 0.125, ((0, 8), (1, 4)), jnp.float32),
        "ffn_gate": centred(seeds[5], (D, FF), D ** -0.5, 0.125, ((0, 8), (1, 4)), jnp.float32),
        "ffn_down": centred(seeds[6], (FF, D), FF ** -0.5, 0.078125, ((0, 4), (1, 8)), jnp.float32),
        "conv_weight": centred(seeds[7], (3, FF), 3 ** -0.5, 3.5, ((1, 4),), jnp.float32),
        "conv_bias": centred(seeds[8], (FF,), 0.5, 3.0, ((0, 4),), jnp.float32),
        "pool_in_scale": jnp.clip(jnp.exp(jax.random.uniform(seeds[9], (D_POOL,), jnp.float32, math.log(0.5), math.log(2.0))), 0.5, 2.0),
        "pool_mix_scale": jnp.clip(jnp.exp(math.log(2.0) - 1.3862944 * jax.random.uniform(seeds[10], (D_POOL,), jnp.float32) ** block_levels(seeds[10], (D_POOL,), ((0, 4),), -0.2, 0.2)), 0.5, 2.0),
        "pool_out_scale": jnp.clip(jnp.exp(math.log(2.0) - 1.3862944 * jax.random.uniform(seeds[11], (D,), jnp.float32) ** block_levels(seeds[11], (D,), ((0, 8),), -0.2, 0.2)), 0.5, 2.0),
        "value_scale": jnp.clip(jnp.exp(math.log(2.0) - 1.3862944 * jax.random.uniform(seeds[12], (FF,), jnp.float32) ** block_levels(seeds[12], (FF,), ((0, 4),), -0.2, 0.2)), 0.5, 2.0),
        "gate_scale": jnp.clip(jnp.exp(math.log(2.0) - 1.3862944 * jax.random.uniform(seeds[13], (FF,), jnp.float32) ** block_levels(seeds[13], (FF,), ((0, 4),), -0.2, 0.2)), 0.5, 2.0),
        "down_scale": jnp.clip(jnp.exp(math.log(2.0) - 1.3862944 * jax.random.uniform(seeds[14], (D,), jnp.float32) ** block_levels(seeds[14], (D,), ((0, 8),), -0.2, 0.2)), 0.5, 2.0),
        "norm1_gain": jnp.clip(1.0 + 0.18 * jax.random.normal(seeds[15], (D,), jnp.float32), 0.1, 1.9),
        "norm1_bias": centred(seeds[16], (D,), 0.5, 3.0, (), jnp.float32),
        "norm2_gain": jnp.clip(1.0 + 0.18 * jax.random.normal(seeds[17], (D,), jnp.float32), 0.1, 1.9),
        "norm2_bias": centred(seeds[18], (D,), 0.5, 3.0, (), jnp.float32),
    }


epsilon = 1e-06
residual_scale = 2.0 ** 0.5
window_spans = (2, 4, 8, 16)

def plain_norm(stream):
    centre = lax.optimization_barrier(jnp.mean(stream, -1, keepdims=True))
    spread = lax.optimization_barrier(jnp.mean(jnp.square(stream - centre), -1, keepdims=True))
    return (stream - centre) * lax.rsqrt(spread + epsilon)

def window_masks(extent):
    places = jnp.arange(extent)
    layers = []
    for window in window_spans:
        window_low = jnp.maximum(places - window // 2, 0)
        window_high = jnp.minimum(places + window // 2, extent)
        inside = (places[None, :] >= window_low[:, None]) & (places[None, :] < window_high[:, None])
        layers.append(inside)
    stacked = jnp.stack(layers).astype(jnp.float32)
    return (stacked, lax.optimization_barrier(jnp.sum(stacked, -1)))

def conv_rows(gate_cells, conv_weight, conv_bias):
    padded = jnp.pad(gate_cells, ((0, 0), (1, 1), (0, 0)))
    return conv_weight[0] * padded[:, :-2] + conv_weight[1] * gate_cells + conv_weight[2] * padded[:, 2:] + conv_bias

def pool_branch(values, pool_mix, mix_scale):
    token_count, pool_width = values.shape
    group_width = pool_width // 4
    cells = values.reshape(token_count // GRID, GRID, 4, group_width).astype(jnp.float32)
    inside, counts = window_masks(GRID)
    totals = jnp.einsum('gpq,rqgc->rpgc', inside, cells)
    averages = totals / jnp.transpose(counts)[None, :, :, None]
    deviation = (averages - cells).astype(jnp.bfloat16)
    mixing = pool_mix.astype(jnp.bfloat16).reshape(group_width, 4, group_width)
    result = jnp.einsum('rpgc,cgq->rpgq', deviation.astype(jnp.float32), mixing.astype(jnp.float32))
    return (result.reshape(token_count, pool_width) * mix_scale).astype(jnp.bfloat16)

def block_sum(left, right):
    block_width = left.shape[1] // N_TP
    total = jnp.zeros((left.shape[0], right.shape[1]), jnp.float32)
    for block_index in range(N_TP):
        lower = block_index * block_width
        partial_value = jnp.dot(left[:, lower:lower + block_width], right[lower:lower + block_width], preferred_element_type=jnp.float32).astype(jnp.bfloat16)
        total = total + lax.optimization_barrier(partial_value).astype(jnp.float32)
    return total

def layer(tokens, pool_in, pool_mix, pool_out, ffn_value, ffn_gate, ffn_down, conv_weight, conv_bias, pool_in_scale, pool_mix_scale, pool_out_scale, value_scale, gate_scale, down_scale, norm1_gain, norm1_bias, norm2_gain, norm2_bias):
    stream = tokens.astype(jnp.float32)
    normed = plain_norm(stream).astype(jnp.bfloat16)
    values = (jnp.dot(normed, pool_in.astype(jnp.bfloat16), preferred_element_type=jnp.float32) * pool_in_scale).astype(jnp.bfloat16)
    pooled = pool_branch(values, pool_mix, pool_mix_scale)
    mixer_out = block_sum(pooled, pool_out.astype(jnp.bfloat16)) * pool_out_scale
    first = (plain_norm(residual_scale * stream + mixer_out) * norm1_gain + norm1_bias).astype(jnp.bfloat16)
    normed_two = plain_norm(first.astype(jnp.float32)).astype(jnp.bfloat16)
    value = jnp.dot(normed_two, ffn_value.astype(jnp.bfloat16), preferred_element_type=jnp.float32) * value_scale
    gate = jnp.dot(normed_two, ffn_gate.astype(jnp.bfloat16), preferred_element_type=jnp.float32) * gate_scale
    hidden_width = gate.shape[1]
    conv = conv_rows(gate.reshape(-1, GRID, hidden_width), conv_weight, conv_bias).reshape(-1, hidden_width)
    hidden = (value * jax.nn.silu(conv)).astype(jnp.bfloat16)
    ffn_out = block_sum(hidden, ffn_down.astype(jnp.bfloat16)) * down_scale
    return (plain_norm(residual_scale * first.astype(jnp.float32) + ffn_out) * norm2_gain + norm2_bias).astype(jnp.bfloat16)

def reference(tokens, pool_in, pool_mix, pool_out, ffn_value, ffn_gate, ffn_down, conv_weight, conv_bias, pool_in_scale, pool_mix_scale, pool_out_scale, value_scale, gate_scale, down_scale, norm1_gain, norm1_bias, norm2_gain, norm2_bias):
    sequences = tokens.reshape(N_FS, TOK_DEV * N_TP, D)

    def one_sequence(sequence):
        return layer(sequence, pool_in, pool_mix, pool_out, ffn_value, ffn_gate, ffn_down, conv_weight, conv_bias, pool_in_scale, pool_mix_scale, pool_out_scale, value_scale, gate_scale, down_scale, norm1_gain, norm1_bias, norm2_gain, norm2_bias)
    return lax.map(one_sequence, sequences).reshape(TOKENS, D)
```

```python
import jax
import jax.numpy as jnp
from jax import lax
from jax.sharding import PartitionSpec as P

GRID = 64
GROUP = 512
CORES = 2

epsilon = 1e-06
residual_scale = 2.0**0.5
window_spans = (2, 4, 8, 16)
axes = ("fs", "tp")


def plain_norm(stream):
    centre = jnp.mean(stream, -1, keepdims=True)
    spread = jnp.mean(jnp.square(stream - centre), -1, keepdims=True)
    return (stream - centre) * lax.rsqrt(spread + epsilon)


def conv_rows(gate_cells, conv_weight, conv_bias):
    padded = jnp.pad(gate_cells, ((0, 0), (1, 1), (0, 0)))
    return (
        conv_weight[0] * padded[:, :-2]
        + conv_weight[1] * gate_cells
        + conv_weight[2] * padded[:, 2:]
        + conv_bias
    )


def deviation_of(values, window):
    row_count, width = values.shape
    cells = values.reshape(row_count // GRID, GRID, width)
    half = jnp.asarray([span // 2 for span in window_spans], jnp.int32)[window]
    rows = lax.broadcasted_iota(jnp.int32, (GRID, GRID), 0)
    columns = lax.broadcasted_iota(jnp.int32, (GRID, GRID), 1)
    inside = (columns >= rows - half) & (columns < rows + half)
    places = lax.broadcasted_iota(jnp.int32, (GRID, 1), 0)
    count = jnp.minimum(places + half, GRID) - jnp.maximum(places - half, 0)
    totals = jnp.einsum(
        "pq,rqc->rpc", inside.astype(jnp.bfloat16), cells, preferred_element_type=jnp.float32
    )
    averages = totals / count[None].astype(jnp.float32)
    return (averages - cells.astype(jnp.float32)).astype(jnp.bfloat16).reshape(row_count, width)


def gathered_body(
    tokens,
    pool_in,
    pool_mix,
    pool_out,
    ffn_value,
    ffn_gate,
    ffn_down,
    conv_weight,
    conv_bias,
    pool_in_scale,
    pool_mix_scale,
    pool_out_scale,
    value_scale,
    gate_scale,
    down_scale,
    norm1_gain,
    norm1_bias,
    norm2_gain,
    norm2_bias,
):
    place = lax.axis_index("tp")
    own_width = pool_mix.shape[1]
    window = place * own_width // GROUP
    window_start = window * GROUP
    window_columns = lax.dynamic_slice_in_dim(pool_in, window_start, GROUP, 1).astype(jnp.bfloat16)
    scale_window = lax.dynamic_slice_in_dim(pool_in_scale, window_start, GROUP, 0)
    out_scale = lax.all_gather(pool_out_scale, "fs", axis=0, tiled=True)
    final_scale = lax.all_gather(down_scale, "fs", axis=0, tiled=True)
    in_window = lax.all_gather(window_columns, "fs", axis=0, tiled=True)
    out_rows = lax.all_gather(pool_out.astype(jnp.bfloat16), "fs", axis=1, tiled=True)
    value_shard = ffn_value.astype(jnp.bfloat16)
    gate_shard = ffn_gate.astype(jnp.bfloat16)
    down_shard = ffn_down.astype(jnp.bfloat16)
    stream = tokens.astype(jnp.float32)
    normed = plain_norm(stream).astype(jnp.bfloat16)
    values = (
        jnp.dot(
            lax.all_gather(normed, "tp", axis=0, tiled=True),
            in_window,
            preferred_element_type=jnp.float32,
        )
        * scale_window
    ).astype(jnp.bfloat16)
    deviation = deviation_of(values, window)
    pooled = (
        jnp.dot(deviation, pool_mix.astype(jnp.bfloat16), preferred_element_type=jnp.float32)
        * pool_mix_scale
    ).astype(jnp.bfloat16)
    mixer_partial = jnp.dot(pooled, out_rows, preferred_element_type=jnp.float32)
    mixer_out = (
        lax.psum_scatter(
            mixer_partial.astype(jnp.bfloat16), "tp", scatter_dimension=0, tiled=True
        ).astype(jnp.float32)
        * out_scale
    )
    first = (plain_norm(residual_scale * stream + mixer_out) * norm1_gain + norm1_bias).astype(
        jnp.bfloat16
    )
    normed_two = plain_norm(first.astype(jnp.float32)).astype(jnp.bfloat16)
    hidden_width = value_shard.shape[1]
    gathered = lax.all_gather(normed_two, "tp", axis=0, tiled=True)
    value_full = lax.all_gather(value_shard, "fs", axis=0, tiled=True)
    gate_full = lax.all_gather(gate_shard, "fs", axis=0, tiled=True)
    value = jnp.dot(gathered, value_full, preferred_element_type=jnp.float32) * value_scale
    gate = jnp.dot(gathered, gate_full, preferred_element_type=jnp.float32) * gate_scale
    conv = conv_rows(gate.reshape(-1, GRID, hidden_width), conv_weight, conv_bias).reshape(
        -1, hidden_width
    )
    hidden = (value * jax.nn.silu(conv)).astype(jnp.bfloat16)
    down_full = lax.all_gather(down_shard, "fs", axis=1, tiled=True)
    partial_value = jnp.dot(hidden, down_full, preferred_element_type=jnp.float32)
    summed = lax.psum_scatter(
        partial_value.astype(jnp.bfloat16), "tp", scatter_dimension=0, tiled=True
    ).astype(jnp.float32)
    ffn_out = summed * final_scale
    return (
        plain_norm(residual_scale * first.astype(jnp.float32) + ffn_out) * norm2_gain + norm2_bias
    ).astype(jnp.bfloat16)


FLIP_CORE, FLIP_X, FLIP_Y, FLIP_Z1, FLIP_Z2 = 1, 2, 4, 8, 16
PLANE = (0, FLIP_X, FLIP_Y, FLIP_X | FLIP_Y)
SLOTS = 8


def flip(array, mask):
    if mask == 0:
        return array
    return lax.ppermute(array, axes, [(device, device ^ mask) for device in range(32)])


def turn(array):
    def target(device):
        y, core = (device >> 2) & 1, device & 1
        return (device & ~5) | (core << 2) | y

    return lax.ppermute(array, axes, [(device, target(device)) for device in range(32)])


def in_slots(array, key):
    block = array.shape[-1] // SLOTS
    for bit in (1, 2, 4):
        pieces = [array[..., (k ^ bit) * block : ((k ^ bit) + 1) * block] for k in range(SLOTS)]
        array = jnp.where((key & bit) != 0, jnp.concatenate(pieces, -1), array)
    return array


def spread_over_z(piece):
    one = flip(piece, FLIP_Z1)
    two = flip(piece, FLIP_Z2)
    three = flip(two, FLIP_Z1)
    blocks = []
    for own in (piece, one, two, three):
        blocks += [own, flip(own, FLIP_CORE)]
    return blocks


def to_plane(array):
    return jnp.concatenate([flip(array, mask) for mask in PLANE], 0)


def from_plane(partial):
    rows = partial.shape[0] // len(PLANE)
    pieces = [flip(partial[j * rows : (j + 1) * rows], mask) for j, mask in enumerate(PLANE)]
    total = pieces[0].astype(jnp.float32)
    for piece in pieces[1:]:
        total = total + piece.astype(jnp.float32)
    return total


def dot_blocks(left, blocks):
    width = blocks[0].shape[0]
    total = None
    for k, block in enumerate(blocks):
        part = jnp.dot(
            left[:, k * width : (k + 1) * width], block, preferred_element_type=jnp.float32
        )
        total = part if total is None else total + part
    return total


def exchange_body(
    tokens,
    pool_in,
    pool_mix,
    pool_out,
    ffn_value,
    ffn_gate,
    ffn_down,
    conv_weight,
    conv_bias,
    pool_in_scale,
    pool_mix_scale,
    pool_out_scale,
    value_scale,
    gate_scale,
    down_scale,
    norm1_gain,
    norm1_bias,
    norm2_gain,
    norm2_bias,
):
    half = jnp.bfloat16
    fs, tp = lax.axis_index("fs"), lax.axis_index("tp")
    z, y, x, core = fs >> 1, fs & 1, tp >> 1, tp & 1
    key = z * 2 + core
    own_width = pool_mix.shape[1]
    in_piece = turn(lax.dynamic_slice_in_dim(pool_in, tp * own_width, own_width, 1).astype(half))
    out_piece = turn((pool_out * pool_out_scale).astype(half))
    value_piece = turn(ffn_value.astype(half))
    gate_piece = turn(ffn_gate.astype(half))
    down_piece = turn((ffn_down * down_scale).astype(half))
    unit_rows = turn(
        jnp.concatenate([conv_weight, conv_bias[None], value_scale[None], gate_scale[None]], 0)
    )
    mix_own = pool_mix.astype(half)
    mix = jnp.where(core == y, mix_own, flip(mix_own, FLIP_CORE))
    mix_scale = jnp.where(core == y, pool_mix_scale, flip(pool_mix_scale, FLIP_CORE))
    window = x * 2 + y
    scale_window = lax.dynamic_slice_in_dim(pool_in_scale, window * own_width, own_width, 0)

    stream = in_slots(tokens, key).astype(jnp.float32)
    normed = to_plane(plain_norm(stream).astype(half))
    in_blocks = spread_over_z(in_piece)
    out_blocks = spread_over_z(out_piece)
    values = (dot_blocks(normed, in_blocks) * scale_window).astype(half)
    deviation = deviation_of(values, window)
    pooled = (jnp.dot(deviation, mix, preferred_element_type=jnp.float32) * mix_scale).astype(half)
    mixer_partial = jnp.concatenate(
        [jnp.dot(pooled, b, preferred_element_type=jnp.float32).astype(half) for b in out_blocks], 1
    )
    mixer_out = from_plane(mixer_partial)
    gain1, bias1 = in_slots(norm1_gain, key), in_slots(norm1_bias, key)
    gain2, bias2 = in_slots(norm2_gain, key), in_slots(norm2_bias, key)
    first = (plain_norm(residual_scale * stream + mixer_out) * gain1 + bias1).astype(half)
    normed_two = to_plane(plain_norm(first.astype(jnp.float32)).astype(half))

    value_blocks = spread_over_z(value_piece)
    gate_blocks = spread_over_z(gate_piece)
    down_blocks = spread_over_z(down_piece)
    gate = dot_blocks(normed_two, gate_blocks) * unit_rows[5]
    value = dot_blocks(normed_two, value_blocks) * unit_rows[4]
    hidden_width = gate.shape[1]
    conv = conv_rows(gate.reshape(-1, GRID, hidden_width), unit_rows[:3], unit_rows[3])
    hidden = (value * jax.nn.silu(conv.reshape(-1, hidden_width))).astype(half)
    sums = []
    for s in range(0, SLOTS, 2):
        pair = [
            jnp.dot(hidden, b, preferred_element_type=jnp.float32).astype(half)
            for b in down_blocks[s : s + 2]
        ]
        sums.append(from_plane(jnp.concatenate(pair, 1)))
    ffn_out = jnp.concatenate(sums, 1)
    last = plain_norm(residual_scale * first.astype(jnp.float32) + ffn_out) * gain2 + bias2
    return in_slots(last.astype(half), key)


def solution(mesh):
    placed = (
        P(("fs", "tp"), None),
        P("fs", None),
        P(None, "tp"),
        P("tp", "fs"),
        P("fs", "tp"),
        P("fs", "tp"),
        P("tp", "fs"),
        P(None, "tp"),
        P("tp"),
        P(),
        P("tp"),
        P("fs"),
        P("tp"),
        P("tp"),
        P("fs"),
        P(),
        P(),
        P(),
        P(),
    )
    chips_fs, chips_tp = mesh.shape["fs"], mesh.shape["tp"] // CORES
    plain = chips_fs == SLOTS and chips_tp == CORES
    return jax.shard_map(
        exchange_body if plain else gathered_body,
        mesh=mesh,
        in_specs=placed,
        out_specs=P(("fs", "tp"), None),
        check_vma=False,
    )
```

```python
import jax
import jax.numpy as jnp
from jax import lax
from jax.sharding import PartitionSpec as P

GRID = 64
GROUP = 512
CORES = 2

epsilon = 1e-06
residual_scale = 2.0**0.5
window_spans = (2, 4, 8, 16)
axes = ("fs", "tp")


def plain_norm(stream):
    centre = jnp.mean(stream, -1, keepdims=True)
    spread = jnp.mean(jnp.square(stream - centre), -1, keepdims=True)
    return (stream - centre) * lax.rsqrt(spread + epsilon)


def conv_rows(gate_cells, conv_weight, conv_bias):
    padded = jnp.pad(gate_cells, ((0, 0), (1, 1), (0, 0)))
    return (
        conv_weight[0] * padded[:, :-2]
        + conv_weight[1] * gate_cells
        + conv_weight[2] * padded[:, 2:]
        + conv_bias
    )


def window_mask(window):
    half = jnp.int32(window_spans[0] // 2)
    for place, span in enumerate(window_spans):
        half = jnp.where(window == place, span // 2, half)
    rows = lax.broadcasted_iota(jnp.int32, (GRID, GRID), 0)
    columns = lax.broadcasted_iota(jnp.int32, (GRID, GRID), 1)
    inside = (columns >= rows - half) & (columns < rows + half)
    places = lax.broadcasted_iota(jnp.int32, (GRID, 1), 0)
    count = jnp.minimum(places + half, GRID) - jnp.maximum(places - half, 0)
    return inside.astype(jnp.bfloat16), count.astype(jnp.float32)


def deviation_of(values, mask):
    row_count, width = values.shape
    cells = values.reshape(row_count // GRID, GRID, width)
    inside, count = mask
    totals = jnp.einsum("pq,rqc->rpc", inside, cells, preferred_element_type=jnp.float32)
    averages = totals / count[None]
    return (averages - cells.astype(jnp.float32)).astype(jnp.bfloat16).reshape(row_count, width)


def gathered_body(
    tokens,
    pool_in,
    pool_mix,
    pool_out,
    ffn_value,
    ffn_gate,
    ffn_down,
    conv_weight,
    conv_bias,
    pool_in_scale,
    pool_mix_scale,
    pool_out_scale,
    value_scale,
    gate_scale,
    down_scale,
    norm1_gain,
    norm1_bias,
    norm2_gain,
    norm2_bias,
):
    place = lax.axis_index("tp")
    own_width = pool_mix.shape[1]
    window = place * own_width // GROUP
    window_start = window * GROUP
    window_columns = lax.dynamic_slice_in_dim(pool_in, window_start, GROUP, 1).astype(jnp.bfloat16)
    scale_window = lax.dynamic_slice_in_dim(pool_in_scale, window_start, GROUP, 0)
    out_scale = lax.all_gather(pool_out_scale, "fs", axis=0, tiled=True)
    final_scale = lax.all_gather(down_scale, "fs", axis=0, tiled=True)
    in_window = lax.all_gather(window_columns, "fs", axis=0, tiled=True)
    out_rows = lax.all_gather(pool_out.astype(jnp.bfloat16), "fs", axis=1, tiled=True)
    value_shard = ffn_value.astype(jnp.bfloat16)
    gate_shard = ffn_gate.astype(jnp.bfloat16)
    down_shard = ffn_down.astype(jnp.bfloat16)
    stream = tokens.astype(jnp.float32)
    normed = plain_norm(stream).astype(jnp.bfloat16)
    values = (
        jnp.dot(
            lax.all_gather(normed, "tp", axis=0, tiled=True),
            in_window,
            preferred_element_type=jnp.float32,
        )
        * scale_window
    ).astype(jnp.bfloat16)
    deviation = deviation_of(values, window_mask(window))
    pooled = (
        jnp.dot(deviation, pool_mix.astype(jnp.bfloat16), preferred_element_type=jnp.float32)
        * pool_mix_scale
    ).astype(jnp.bfloat16)
    mixer_partial = jnp.dot(pooled, out_rows, preferred_element_type=jnp.float32)
    mixer_out = (
        lax.psum_scatter(
            mixer_partial.astype(jnp.bfloat16), "tp", scatter_dimension=0, tiled=True
        ).astype(jnp.float32)
        * out_scale
    )
    first = (plain_norm(residual_scale * stream + mixer_out) * norm1_gain + norm1_bias).astype(
        jnp.bfloat16
    )
    normed_two = plain_norm(first.astype(jnp.float32)).astype(jnp.bfloat16)
    hidden_width = value_shard.shape[1]
    gathered = lax.all_gather(normed_two, "tp", axis=0, tiled=True)
    value_full = lax.all_gather(value_shard, "fs", axis=0, tiled=True)
    gate_full = lax.all_gather(gate_shard, "fs", axis=0, tiled=True)
    value = jnp.dot(gathered, value_full, preferred_element_type=jnp.float32) * value_scale
    gate = jnp.dot(gathered, gate_full, preferred_element_type=jnp.float32) * gate_scale
    conv = conv_rows(gate.reshape(-1, GRID, hidden_width), conv_weight, conv_bias).reshape(
        -1, hidden_width
    )
    hidden = (value * jax.nn.silu(conv)).astype(jnp.bfloat16)
    down_full = lax.all_gather(down_shard, "fs", axis=1, tiled=True)
    partial_value = jnp.dot(hidden, down_full, preferred_element_type=jnp.float32)
    summed = lax.psum_scatter(
        partial_value.astype(jnp.bfloat16), "tp", scatter_dimension=0, tiled=True
    ).astype(jnp.float32)
    ffn_out = summed * final_scale
    return (
        plain_norm(residual_scale * first.astype(jnp.float32) + ffn_out) * norm2_gain + norm2_bias
    ).astype(jnp.bfloat16)


FLIP_CORE, FLIP_X, FLIP_Y, FLIP_Z1, FLIP_Z2 = 1, 2, 4, 8, 16
SLOTS = 8


def flip(array, mask):
    return lax.ppermute(array, axes, [(device, device ^ mask) for device in range(32)])


def turn(array, stays):
    pairs = [(d, d ^ 5) for d in range(32) if ((d >> 2) & 1) != (d & 1)]
    moved = lax.ppermute(array, axes, pairs)
    return jnp.where(stays, array, moved)


def in_place(blocks, key, axis):
    size = blocks[0].shape[axis]
    shape = list(blocks[0].shape)
    shape[axis] = size * len(blocks)
    whole = jnp.zeros(shape, blocks[0].dtype)
    for k, block in enumerate(blocks):
        whole = lax.dynamic_update_slice_in_dim(whole, block, (k ^ key) * size, axis)
    return whole


def with_other_core(pieces):
    blocks = []
    for own in pieces:
        blocks += [own, flip(own, FLIP_CORE)]
    return blocks


def spread_over_z(piece):
    one = flip(piece, FLIP_Z1)
    two = flip(piece, FLIP_Z2)
    three = flip(two, FLIP_Z1)
    return with_other_core([piece, one, two, three])


def deal_over_z(even, odd):
    one = flip(odd, FLIP_Z1)
    two = flip(even, FLIP_Z2)
    three = flip(odd, FLIP_Z1 | FLIP_Z2)
    return with_other_core([even, one, two, three])


def to_plane(array):
    middle = array.shape[0] // 2
    by_x = flip(array, FLIP_X)
    by_y = flip(array, FLIP_Y)
    upper = flip(by_y[:middle], FLIP_X)
    lower = flip(by_x[middle:], FLIP_Y)
    return jnp.concatenate([array, by_x, by_y, upper, lower], 0)


def dot(left, right):
    return jnp.dot(left, right, preferred_element_type=jnp.float32)


def dot_blocks(left, blocks, key):
    width = blocks[0].shape[0]
    total = None
    for k, block in enumerate(blocks):
        columns = lax.dynamic_slice_in_dim(left, (k ^ key) * width, width, 1)
        part = dot(columns, block)
        total = part if total is None else total + part
    return total


def hidden_units(left, up_pairs, z, unit_rows):
    both_sums = dot_blocks(left, up_pairs, z)
    cut = both_sums.shape[1] // 2
    value, gate = both_sums[:, :cut], both_sums[:, cut:]
    conv = conv_rows(gate.reshape(-1, GRID, cut), unit_rows[:3], unit_rows[3]).reshape(-1, cut)
    return (value * jax.nn.silu(conv)).astype(jnp.bfloat16)


ORDERS = ((1, 2, 4), (2, 1, 4), (4, 1, 2), (4, 2, 1))


def exchange_body(
    tokens,
    pool_in,
    pool_mix,
    pool_out,
    ffn_value,
    ffn_gate,
    ffn_down,
    conv_weight,
    conv_bias,
    pool_in_scale,
    pool_mix_scale,
    pool_out_scale,
    value_scale,
    gate_scale,
    down_scale,
    norm1_gain,
    norm1_bias,
    norm2_gain,
    norm2_bias,
):
    half = jnp.bfloat16
    fs, tp = lax.axis_index("fs"), lax.axis_index("tp")
    z, y, x, core = fs >> 1, fs & 1, tp >> 1, tp & 1
    key = z * 2 + core
    stays = y == core
    low = (z & 1) == 0
    rows, own_width = tokens.shape[0], pool_mix.shape[1]
    units = ffn_value.shape[1]
    cut = units // 2

    in_own = lax.dynamic_slice_in_dim(pool_in, tp * own_width, own_width, 1)
    in_piece = turn(in_own.astype(half), stays)
    out_piece = turn((pool_out * pool_out_scale).astype(half), stays)
    in_blocks = spread_over_z(in_piece)
    out_blocks = spread_over_z(out_piece)

    stream = tokens.astype(jnp.float32)
    normed_own = plain_norm(stream).astype(half)
    normed_y = flip(normed_own, FLIP_Y)
    normed = jnp.concatenate(
        [normed_own, flip(normed_own, FLIP_X), normed_y, flip(normed_y, FLIP_X)], 0
    )

    value_own = (ffn_value * value_scale).astype(half)
    gate_own = (ffn_gate * gate_scale).astype(half)
    up_own = jnp.concatenate([value_own, gate_own], 1)
    down_own = (ffn_down * down_scale).astype(half)
    up = turn(up_own, stays)
    first_half = jnp.concatenate([up[:, :cut], up[:, units : units + cut]], 1)
    second_half = jnp.concatenate([up[:, cut:units], up[:, units + cut :]], 1)
    up_blocks = deal_over_z(
        jnp.where(low, first_half, second_half), jnp.where(low, second_half, first_half)
    )
    down = turn(down_own, stays)
    down_blocks = deal_over_z(
        jnp.where(low, down[:cut], down[cut:]), jnp.where(low, down[cut:], down[:cut])
    )
    unit_rows = turn(jnp.concatenate([conv_weight, conv_bias[None]], 0), stays)
    unit_rows = jnp.where(low, unit_rows[:, :cut], unit_rows[:, cut:])
    mix_own = (pool_mix * pool_mix_scale).astype(half)
    mix = jnp.where(stays, mix_own, flip(mix_own, FLIP_CORE))
    window = x * 2 + y
    scale_window = lax.dynamic_slice_in_dim(pool_in_scale, window * own_width, own_width, 0)
    mask = window_mask(window)

    values = (dot_blocks(normed, in_blocks, key) * scale_window).astype(half)
    values, *late = lax.optimization_barrier([values] + out_blocks[4:])
    out_blocks = out_blocks[:4] + late
    deviation = deviation_of(values, mask)
    pooled = dot(deviation, mix).astype(half)
    out_full = in_place(out_blocks, key, 1)
    mixer_out = None
    for j in (3, 1, 2, 0):
        partial = dot(pooled[j * rows : (j + 1) * rows], out_full).astype(half)
        if j > 0:
            partial = flip(partial, j * FLIP_X)
        partial = partial.astype(jnp.float32)
        mixer_out = partial if mixer_out is None else mixer_out + partial
    first = (plain_norm(residual_scale * stream + mixer_out) * norm1_gain + norm1_bias).astype(half)
    second = plain_norm(first.astype(jnp.float32)).astype(half)
    second_z = flip(second, FLIP_Z1)
    near, far = to_plane(second), to_plane(second_z)

    up_pairs = [in_place(up_blocks[2 * s : 2 * s + 2], core, 0) for s in range(4)]
    near = hidden_units(near, up_pairs, z, unit_rows)
    near, far = lax.optimization_barrier((near, far))
    far = hidden_units(far, up_pairs, z, unit_rows)

    blocks = [side[j * rows : (j + 1) * rows] for side in (near, far) for j in range(4)]

    def places(start, later):
        one, two = later
        return jnp.concatenate([blocks[start + k] for k in (0, two, one, one + two)], 0)

    sums = [None] * 4
    sent = [None] * 4
    for s, (one, *later) in enumerate(ORDERS):
        arranged = ORDERS[s ^ 1][1:] if one == 4 else later
        parts = [places(one, arranged), places(0, later)] + down_blocks[2 * s : 2 * s + 2]
        away, kept, *pair = lax.optimization_barrier(parts)
        columns = in_place(pair, core, 1)
        sent[s] = flip(dot(away, columns).astype(half), one * FLIP_X)
        sums[s] = (kept, columns)
    for s, (one, two, three) in enumerate(ORDERS):
        total = dot(*sums[s]) + sent[s ^ 1 if one == 4 else s].astype(jnp.float32)
        moved = flip(total[2 * rows :].astype(half), two * FLIP_X)
        sums[s] = total[: 2 * rows] + moved.astype(jnp.float32)
    for s, (_, _, three) in enumerate(ORDERS):
        sent[s] = flip(sums[s][rows:].astype(half), three * FLIP_X)
    for s, (_, _, three) in enumerate(ORDERS):
        sums[s] = sums[s][:rows] + sent[s ^ 1 if three == 4 else s].astype(jnp.float32)
    ffn_out = in_place(sums, z, 1)
    last = plain_norm(residual_scale * first.astype(jnp.float32) + ffn_out) * norm2_gain + norm2_bias
    return last.astype(half)


def solution(mesh):
    placed = (
        P(("fs", "tp"), None),
        P("fs", None),
        P(None, "tp"),
        P("tp", "fs"),
        P("fs", "tp"),
        P("fs", "tp"),
        P("tp", "fs"),
        P(None, "tp"),
        P("tp"),
        P(),
        P("tp"),
        P("fs"),
        P("tp"),
        P("tp"),
        P("fs"),
        P(),
        P(),
        P(),
        P(),
    )
    if mesh.shape["fs"] != SLOTS or mesh.shape["tp"] != 2 * CORES:
        return mapped(gathered_body, mesh, placed)

    return mapped(exchange_body, mesh, placed)


def mapped(body, mesh, placed):
    return jax.shard_map(
        body, mesh=mesh, in_specs=placed, out_specs=P(("fs", "tp"), None), check_vma=False
    )
```

```python
import jax
import jax.numpy as jnp
from jax import lax
from jax.sharding import PartitionSpec as P

GRID = 64
GROUP = 512
CORES = 2

epsilon = 1e-06
residual_scale = 2.0**0.5
window_spans = (2, 4, 8, 16)
axes = ("fs", "tp")


def plain_norm(stream):
    centre = jnp.mean(stream, -1, keepdims=True)
    spread = jnp.mean(jnp.square(stream - centre), -1, keepdims=True)
    return (stream - centre) * lax.rsqrt(spread + epsilon)


def conv_rows(gate_cells, conv_weight, conv_bias):
    padded = jnp.pad(gate_cells, ((0, 0), (1, 1), (0, 0)))
    return (
        conv_weight[0] * padded[:, :-2]
        + conv_weight[1] * gate_cells
        + conv_weight[2] * padded[:, 2:]
        + conv_bias
    )


def window_mask(window):
    half = jnp.int32(window_spans[0] // 2)
    for place, span in enumerate(window_spans):
        half = jnp.where(window == place, span // 2, half)
    rows = lax.broadcasted_iota(jnp.int32, (GRID, GRID), 0)
    columns = lax.broadcasted_iota(jnp.int32, (GRID, GRID), 1)
    inside = (columns >= rows - half) & (columns < rows + half)
    places = lax.broadcasted_iota(jnp.int32, (GRID, 1), 0)
    count = jnp.minimum(places + half, GRID) - jnp.maximum(places - half, 0)
    return inside.astype(jnp.bfloat16), count.astype(jnp.float32)


def deviation_of(values, mask):
    row_count, width = values.shape
    cells = values.reshape(row_count // GRID, GRID, width)
    inside, count = mask
    totals = jnp.einsum("pq,rqc->rpc", inside, cells, preferred_element_type=jnp.float32)
    averages = totals / count[None]
    return (averages - cells.astype(jnp.float32)).astype(jnp.bfloat16).reshape(row_count, width)


def gathered_body(
    tokens,
    pool_in,
    pool_mix,
    pool_out,
    ffn_value,
    ffn_gate,
    ffn_down,
    conv_weight,
    conv_bias,
    pool_in_scale,
    pool_mix_scale,
    pool_out_scale,
    value_scale,
    gate_scale,
    down_scale,
    norm1_gain,
    norm1_bias,
    norm2_gain,
    norm2_bias,
):
    place = lax.axis_index("tp")
    own_width = pool_mix.shape[1]
    window = place * own_width // GROUP
    window_start = window * GROUP
    window_columns = lax.dynamic_slice_in_dim(pool_in, window_start, GROUP, 1).astype(jnp.bfloat16)
    scale_window = lax.dynamic_slice_in_dim(pool_in_scale, window_start, GROUP, 0)
    out_scale = lax.all_gather(pool_out_scale, "fs", axis=0, tiled=True)
    final_scale = lax.all_gather(down_scale, "fs", axis=0, tiled=True)
    in_window = lax.all_gather(window_columns, "fs", axis=0, tiled=True)
    out_rows = lax.all_gather(pool_out.astype(jnp.bfloat16), "fs", axis=1, tiled=True)
    value_shard = ffn_value.astype(jnp.bfloat16)
    gate_shard = ffn_gate.astype(jnp.bfloat16)
    down_shard = ffn_down.astype(jnp.bfloat16)
    stream = tokens.astype(jnp.float32)
    normed = plain_norm(stream).astype(jnp.bfloat16)
    values = (
        jnp.dot(
            lax.all_gather(normed, "tp", axis=0, tiled=True),
            in_window,
            preferred_element_type=jnp.float32,
        )
        * scale_window
    ).astype(jnp.bfloat16)
    deviation = deviation_of(values, window_mask(window))
    pooled = (
        jnp.dot(deviation, pool_mix.astype(jnp.bfloat16), preferred_element_type=jnp.float32)
        * pool_mix_scale
    ).astype(jnp.bfloat16)
    mixer_partial = jnp.dot(pooled, out_rows, preferred_element_type=jnp.float32)
    mixer_out = (
        lax.psum_scatter(
            mixer_partial.astype(jnp.bfloat16), "tp", scatter_dimension=0, tiled=True
        ).astype(jnp.float32)
        * out_scale
    )
    first = (plain_norm(residual_scale * stream + mixer_out) * norm1_gain + norm1_bias).astype(
        jnp.bfloat16
    )
    normed_two = plain_norm(first.astype(jnp.float32)).astype(jnp.bfloat16)
    hidden_width = value_shard.shape[1]
    gathered = lax.all_gather(normed_two, "tp", axis=0, tiled=True)
    value_full = lax.all_gather(value_shard, "fs", axis=0, tiled=True)
    gate_full = lax.all_gather(gate_shard, "fs", axis=0, tiled=True)
    value = jnp.dot(gathered, value_full, preferred_element_type=jnp.float32) * value_scale
    gate = jnp.dot(gathered, gate_full, preferred_element_type=jnp.float32) * gate_scale
    conv = conv_rows(gate.reshape(-1, GRID, hidden_width), conv_weight, conv_bias).reshape(
        -1, hidden_width
    )
    hidden = (value * jax.nn.silu(conv)).astype(jnp.bfloat16)
    down_full = lax.all_gather(down_shard, "fs", axis=1, tiled=True)
    partial_value = jnp.dot(hidden, down_full, preferred_element_type=jnp.float32)
    summed = lax.psum_scatter(
        partial_value.astype(jnp.bfloat16), "tp", scatter_dimension=0, tiled=True
    ).astype(jnp.float32)
    ffn_out = summed * final_scale
    return (
        plain_norm(residual_scale * first.astype(jnp.float32) + ffn_out) * norm2_gain + norm2_bias
    ).astype(jnp.bfloat16)


FLIP_CORE, FLIP_X, FLIP_Y, FLIP_Z1, FLIP_Z2 = 1, 2, 4, 8, 16
SLOTS = 8


def flip(array, mask):
    return lax.ppermute(array, axes, [(device, device ^ mask) for device in range(32)])


def turn(array, stays):
    pairs = [(d, d ^ 5) for d in range(32) if ((d >> 2) & 1) != (d & 1)]
    moved = lax.ppermute(array, axes, pairs)
    return jnp.where(stays, array, moved)


def in_place(blocks, key, axis):
    size = blocks[0].shape[axis]
    shape = list(blocks[0].shape)
    shape[axis] = size * len(blocks)
    whole = jnp.zeros(shape, blocks[0].dtype)
    for k, block in enumerate(blocks):
        whole = lax.dynamic_update_slice_in_dim(whole, block, (k ^ key) * size, axis)
    return whole


def with_other_core(pieces):
    blocks = []
    for own in pieces:
        blocks += [own, flip(own, FLIP_CORE)]
    return blocks


def spread_over_z(piece):
    one = flip(piece, FLIP_Z1)
    two = flip(piece, FLIP_Z2)
    three = flip(two, FLIP_Z1)
    return with_other_core([piece, one, two, three])


def deal_over_z(even, odd):
    one = flip(odd, FLIP_Z1)
    two = flip(even, FLIP_Z2)
    three = flip(odd, FLIP_Z1 | FLIP_Z2)
    return with_other_core([even, one, two, three])


def to_plane(array):
    middle = array.shape[0] // 2
    by_x = flip(array, FLIP_X)
    by_y = flip(array, FLIP_Y)
    upper = flip(by_y[:middle], FLIP_X)
    lower = flip(by_x[middle:], FLIP_Y)
    return jnp.concatenate([array, by_x, by_y, upper, lower], 0)


def dot(left, right):
    return jnp.dot(left, right, preferred_element_type=jnp.float32)


def dot_blocks(left, blocks, key):
    width = blocks[0].shape[0]
    total = None
    for k, block in enumerate(blocks):
        columns = lax.dynamic_slice_in_dim(left, (k ^ key) * width, width, 1)
        part = dot(columns, block)
        total = part if total is None else total + part
    return total


def hidden_units(left, up_pairs, z, unit_rows):
    both_sums = dot_blocks(left, up_pairs, z)
    cut = both_sums.shape[1] // 2
    value, gate = both_sums[:, :cut], both_sums[:, cut:]
    conv = conv_rows(gate.reshape(-1, GRID, cut), unit_rows[:3], unit_rows[3]).reshape(-1, cut)
    return (value * jax.nn.silu(conv)).astype(jnp.bfloat16)


ORDERS = ((1, 2, 4), (2, 1, 4), (1, 2, 4), (2, 1, 4))


def exchange_body(
    tokens,
    pool_in,
    pool_mix,
    pool_out,
    ffn_value,
    ffn_gate,
    ffn_down,
    conv_weight,
    conv_bias,
    pool_in_scale,
    pool_mix_scale,
    pool_out_scale,
    value_scale,
    gate_scale,
    down_scale,
    norm1_gain,
    norm1_bias,
    norm2_gain,
    norm2_bias,
):
    half = jnp.bfloat16
    fs, tp = lax.axis_index("fs"), lax.axis_index("tp")
    z, y, x, core = fs >> 1, fs & 1, tp >> 1, tp & 1
    key = z * 2 + core
    stays = y == core
    low = (z & 1) == 0
    rows, own_width = tokens.shape[0], pool_mix.shape[1]
    units = ffn_value.shape[1]
    cut = units // 2

    in_own = lax.dynamic_slice_in_dim(pool_in, tp * own_width, own_width, 1)
    in_piece = turn(in_own.astype(half), stays)
    out_piece = turn((pool_out * pool_out_scale).astype(half), stays)
    in_blocks = spread_over_z(in_piece)
    out_blocks = spread_over_z(out_piece)

    stream = tokens.astype(jnp.float32)
    normed_own = plain_norm(stream).astype(half)
    normed_y = flip(normed_own, FLIP_Y)
    normed = jnp.concatenate(
        [normed_own, flip(normed_own, FLIP_X), normed_y, flip(normed_y, FLIP_X)], 0
    )

    value_own = (ffn_value * value_scale).astype(half)
    gate_own = (ffn_gate * gate_scale).astype(half)
    up_own = jnp.concatenate([value_own, gate_own], 1)
    down_own = (ffn_down * down_scale).astype(half)
    up = turn(up_own, stays)
    first_half = jnp.concatenate([up[:, :cut], up[:, units : units + cut]], 1)
    second_half = jnp.concatenate([up[:, cut:units], up[:, units + cut :]], 1)
    up_blocks = deal_over_z(
        jnp.where(low, first_half, second_half), jnp.where(low, second_half, first_half)
    )
    down = turn(down_own, stays)
    down_blocks = deal_over_z(
        jnp.where(low, down[:cut], down[cut:]), jnp.where(low, down[cut:], down[:cut])
    )
    unit_rows = jnp.concatenate([conv_weight, conv_bias[None]], 0)
    unit_rows = turn(unit_rows, stays)
    unit_rows = jnp.where(low, unit_rows[:, :cut], unit_rows[:, cut:])
    mix_own = (pool_mix * pool_mix_scale).astype(half)
    mix = jnp.where(stays, mix_own, flip(mix_own, FLIP_CORE))
    window = x * 2 + y
    scale_window = lax.dynamic_slice_in_dim(pool_in_scale, window * own_width, own_width, 0)
    mask = window_mask(window)

    values = (dot_blocks(normed, in_blocks, key) * scale_window).astype(half)
    values, *late = lax.optimization_barrier([values] + out_blocks[4:])
    out_blocks = out_blocks[:4] + late
    deviation = deviation_of(values, mask)
    pooled = dot(deviation, mix).astype(half)
    out_full = in_place(out_blocks, key, 1)
    mixer_out = None
    for j in (3, 1, 2, 0):
        partial = dot(pooled[j * rows : (j + 1) * rows], out_full).astype(half)
        if j > 0:
            partial = flip(partial, j * FLIP_X)
        partial = partial.astype(jnp.float32)
        mixer_out = partial if mixer_out is None else mixer_out + partial
    first = (plain_norm(residual_scale * stream + mixer_out) * norm1_gain + norm1_bias).astype(half)
    second = plain_norm(first.astype(jnp.float32)).astype(half)
    second_z = flip(second, FLIP_Z1)
    near, far = to_plane(second), to_plane(second_z)

    up_blocks[6:] = lax.optimization_barrier([near] + up_blocks[6:])[1:]
    up_pairs = [in_place(up_blocks[2 * s : 2 * s + 2], core, 0) for s in range(4)]
    near = hidden_units(near, up_pairs, z, unit_rows)
    far = hidden_units(far, up_pairs, z, unit_rows)

    blocks = [side[j * rows : (j + 1) * rows] for side in (near, far) for j in range(4)]

    def places(start, later):
        one, two = later
        return jnp.concatenate([blocks[start + k] for k in (0, two, one, one + two)], 0)

    sums = [None] * 4
    sent = [None] * 4
    for s, (one, *later) in enumerate(ORDERS):
        arranged = ORDERS[s ^ 1][1:] if one == 4 else later
        parts = [places(one, arranged), places(0, later)] + down_blocks[2 * s : 2 * s + 2]
        away, kept, *pair = lax.optimization_barrier(parts)
        columns = in_place(pair, core, 1)
        sent[s] = flip(dot(away, columns).astype(half), one * FLIP_X)
        sums[s] = (kept, columns)
    for s, (one, two, three) in enumerate(ORDERS):
        total = dot(*sums[s]) + sent[s ^ 1 if one == 4 else s].astype(jnp.float32)
        moved = flip(total[2 * rows :].astype(half), two * FLIP_X)
        sums[s] = total[: 2 * rows] + moved.astype(jnp.float32)
    for s, (_, _, three) in enumerate(ORDERS):
        sent[s] = flip(sums[s][rows:].astype(half), three * FLIP_X)
    for s, (_, _, three) in enumerate(ORDERS):
        sums[s] = sums[s][:rows] + sent[s ^ 1 if three == 4 else s].astype(jnp.float32)
    ffn_out = in_place(sums, z, 1)
    last = plain_norm(residual_scale * first.astype(jnp.float32) + ffn_out) * norm2_gain + norm2_bias
    return last.astype(half)


def solution(mesh):
    placed = (
        P(("fs", "tp"), None),
        P("fs", None),
        P(None, "tp"),
        P("tp", "fs"),
        P("fs", "tp"),
        P("fs", "tp"),
        P("tp", "fs"),
        P(None, "tp"),
        P("tp"),
        P(),
        P("tp"),
        P("fs"),
        P("tp"),
        P("tp"),
        P("fs"),
        P(),
        P(),
        P(),
        P(),
    )
    if mesh.shape["fs"] != SLOTS or mesh.shape["tp"] != 2 * CORES:
        return mapped(gathered_body, mesh, placed)

    return mapped(exchange_body, mesh, placed)


def mapped(body, mesh, placed):
    return jax.shard_map(
        body, mesh=mesh, in_specs=placed, out_specs=P(("fs", "tp"), None), check_vma=False
    )
```

```python
import jax
import jax.numpy as jnp
from jax import lax
from jax.sharding import PartitionSpec as P

GRID = 64
GROUP = 512
CORES = 2

epsilon = 1e-06
residual_scale = 2.0**0.5
window_spans = (2, 4, 8, 16)
axes = ("fs", "tp")


def plain_norm(stream):
    centre = jnp.mean(stream, -1, keepdims=True)
    spread = jnp.mean(jnp.square(stream - centre), -1, keepdims=True)
    return (stream - centre) * lax.rsqrt(spread + epsilon)


def conv_rows(gate_cells, conv_weight, conv_bias):
    padded = jnp.pad(gate_cells, ((0, 0), (1, 1), (0, 0)))
    return (
        conv_weight[0] * padded[:, :-2]
        + conv_weight[1] * gate_cells
        + conv_weight[2] * padded[:, 2:]
        + conv_bias
    )


def window_mask(window):
    half = jnp.int32(window_spans[0] // 2)
    for place, span in enumerate(window_spans):
        half = jnp.where(window == place, span // 2, half)
    rows = lax.broadcasted_iota(jnp.int32, (GRID, GRID), 0)
    columns = lax.broadcasted_iota(jnp.int32, (GRID, GRID), 1)
    inside = (columns >= rows - half) & (columns < rows + half)
    places = lax.broadcasted_iota(jnp.int32, (GRID, 1), 0)
    count = jnp.minimum(places + half, GRID) - jnp.maximum(places - half, 0)
    return inside.astype(jnp.bfloat16), count.astype(jnp.float32)


def deviation_of(values, mask):
    row_count, width = values.shape
    cells = values.reshape(row_count // GRID, GRID, width)
    inside, count = mask
    totals = jnp.einsum("pq,rqc->rpc", inside, cells, preferred_element_type=jnp.float32)
    averages = totals / count[None]
    return (averages - cells.astype(jnp.float32)).astype(jnp.bfloat16).reshape(row_count, width)


def gathered_body(
    tokens,
    pool_in,
    pool_mix,
    pool_out,
    ffn_value,
    ffn_gate,
    ffn_down,
    conv_weight,
    conv_bias,
    pool_in_scale,
    pool_mix_scale,
    pool_out_scale,
    value_scale,
    gate_scale,
    down_scale,
    norm1_gain,
    norm1_bias,
    norm2_gain,
    norm2_bias,
):
    place = lax.axis_index("tp")
    own_width = pool_mix.shape[1]
    window = place * own_width // GROUP
    window_start = window * GROUP
    window_columns = lax.dynamic_slice_in_dim(pool_in, window_start, GROUP, 1).astype(jnp.bfloat16)
    scale_window = lax.dynamic_slice_in_dim(pool_in_scale, window_start, GROUP, 0)
    out_scale = lax.all_gather(pool_out_scale, "fs", axis=0, tiled=True)
    final_scale = lax.all_gather(down_scale, "fs", axis=0, tiled=True)
    in_window = lax.all_gather(window_columns, "fs", axis=0, tiled=True)
    out_rows = lax.all_gather(pool_out.astype(jnp.bfloat16), "fs", axis=1, tiled=True)
    value_shard = ffn_value.astype(jnp.bfloat16)
    gate_shard = ffn_gate.astype(jnp.bfloat16)
    down_shard = ffn_down.astype(jnp.bfloat16)
    stream = tokens.astype(jnp.float32)
    normed = plain_norm(stream).astype(jnp.bfloat16)
    values = (
        jnp.dot(
            lax.all_gather(normed, "tp", axis=0, tiled=True),
            in_window,
            preferred_element_type=jnp.float32,
        )
        * scale_window
    ).astype(jnp.bfloat16)
    deviation = deviation_of(values, window_mask(window))
    pooled = (
        jnp.dot(deviation, pool_mix.astype(jnp.bfloat16), preferred_element_type=jnp.float32)
        * pool_mix_scale
    ).astype(jnp.bfloat16)
    mixer_partial = jnp.dot(pooled, out_rows, preferred_element_type=jnp.float32)
    mixer_out = (
        lax.psum_scatter(
            mixer_partial.astype(jnp.bfloat16), "tp", scatter_dimension=0, tiled=True
        ).astype(jnp.float32)
        * out_scale
    )
    first = (plain_norm(residual_scale * stream + mixer_out) * norm1_gain + norm1_bias).astype(
        jnp.bfloat16
    )
    normed_two = plain_norm(first.astype(jnp.float32)).astype(jnp.bfloat16)
    hidden_width = value_shard.shape[1]
    gathered = lax.all_gather(normed_two, "tp", axis=0, tiled=True)
    value_full = lax.all_gather(value_shard, "fs", axis=0, tiled=True)
    gate_full = lax.all_gather(gate_shard, "fs", axis=0, tiled=True)
    value = jnp.dot(gathered, value_full, preferred_element_type=jnp.float32) * value_scale
    gate = jnp.dot(gathered, gate_full, preferred_element_type=jnp.float32) * gate_scale
    conv = conv_rows(gate.reshape(-1, GRID, hidden_width), conv_weight, conv_bias).reshape(
        -1, hidden_width
    )
    hidden = (value * jax.nn.silu(conv)).astype(jnp.bfloat16)
    down_full = lax.all_gather(down_shard, "fs", axis=1, tiled=True)
    partial_value = jnp.dot(hidden, down_full, preferred_element_type=jnp.float32)
    summed = lax.psum_scatter(
        partial_value.astype(jnp.bfloat16), "tp", scatter_dimension=0, tiled=True
    ).astype(jnp.float32)
    ffn_out = summed * final_scale
    return (
        plain_norm(residual_scale * first.astype(jnp.float32) + ffn_out) * norm2_gain + norm2_bias
    ).astype(jnp.bfloat16)


FLIP_CORE, FLIP_X, FLIP_Y, FLIP_Z1, FLIP_Z2 = 1, 2, 4, 8, 16
SLOTS = 8


def flip(array, mask):
    return lax.ppermute(array, axes, [(device, device ^ mask) for device in range(32)])


def turn(array, stays):
    pairs = [(d, d ^ 5) for d in range(32) if ((d >> 2) & 1) != (d & 1)]
    moved = lax.ppermute(array, axes, pairs)
    return jnp.where(stays, array, moved)


def in_place(blocks, key, axis):
    size = blocks[0].shape[axis]
    shape = list(blocks[0].shape)
    shape[axis] = size * len(blocks)
    whole = jnp.zeros(shape, blocks[0].dtype)
    for k, block in enumerate(blocks):
        whole = lax.dynamic_update_slice_in_dim(whole, block, (k ^ key) * size, axis)
    return whole


def with_other_core(pieces):
    blocks = []
    for own in pieces:
        blocks += [own, flip(own, FLIP_CORE)]
    return blocks


def spread_over_z(piece):
    one = flip(piece, FLIP_Z1)
    two = flip(piece, FLIP_Z2)
    three = flip(two, FLIP_Z1)
    return with_other_core([piece, one, two, three])


def deal_over_z(even, odd):
    one = flip(odd, FLIP_Z1)
    two = flip(even, FLIP_Z2)
    three = flip(odd, FLIP_Z1 | FLIP_Z2)
    return with_other_core([even, one, two, three])


def to_plane(array):
    middle = array.shape[0] // 2
    by_x = flip(array, FLIP_X)
    by_y = flip(array, FLIP_Y)
    upper = flip(by_y[:middle], FLIP_X)
    lower = flip(by_x[middle:], FLIP_Y)
    return [array, by_x, by_y, upper, lower]


def dot(left, right):
    return jnp.dot(left, right, preferred_element_type=jnp.float32)


def dot_blocks(left, blocks, key):
    width = blocks[0].shape[0]
    total = None
    for k, block in enumerate(blocks):
        columns = lax.dynamic_slice_in_dim(left, (k ^ key) * width, width, 1)
        part = dot(columns, block)
        total = part if total is None else total + part
    return total


def hidden_units(left, up_pairs, z, unit_rows):
    both_sums = dot_blocks(left, up_pairs, z)
    cut = both_sums.shape[1] // 2
    value, gate = both_sums[:, :cut], both_sums[:, cut:]
    conv = conv_rows(gate.reshape(-1, GRID, cut), unit_rows[:3], unit_rows[3]).reshape(-1, cut)
    return (value * jax.nn.silu(conv)).astype(jnp.bfloat16)


ORDERS = ((1, 2, 4), (2, 1, 4), (1, 2, 4), (2, 1, 4))


def exchange_body(
    tokens,
    pool_in,
    pool_mix,
    pool_out,
    ffn_value,
    ffn_gate,
    ffn_down,
    conv_weight,
    conv_bias,
    pool_in_scale,
    pool_mix_scale,
    pool_out_scale,
    value_scale,
    gate_scale,
    down_scale,
    norm1_gain,
    norm1_bias,
    norm2_gain,
    norm2_bias,
):
    half = jnp.bfloat16
    fs, tp = lax.axis_index("fs"), lax.axis_index("tp")
    z, y, x, core = fs >> 1, fs & 1, tp >> 1, tp & 1
    key = z * 2 + core
    stays = y == core
    low = (z & 1) == 0
    rows, own_width = tokens.shape[0], pool_mix.shape[1]
    units = ffn_value.shape[1]
    cut = units // 2

    in_own = lax.dynamic_slice_in_dim(pool_in, tp * own_width, own_width, 1)
    in_piece = turn(in_own.astype(half), stays)
    out_piece = turn((pool_out * pool_out_scale).astype(half), stays)
    in_blocks = spread_over_z(in_piece)
    out_blocks = spread_over_z(out_piece)

    stream = tokens.astype(jnp.float32)
    normed_own = plain_norm(stream).astype(half)
    normed_y = flip(normed_own, FLIP_Y)
    normed = jnp.concatenate(
        [normed_own, flip(normed_own, FLIP_X), normed_y, flip(normed_y, FLIP_X)], 0
    )

    value_own = (ffn_value * value_scale).astype(half)
    gate_own = (ffn_gate * gate_scale).astype(half)
    up_own = jnp.concatenate([value_own, gate_own], 1)
    down_own = (ffn_down * down_scale).astype(half)
    up = turn(up_own, stays)
    first_half = jnp.concatenate([up[:, :cut], up[:, units : units + cut]], 1)
    second_half = jnp.concatenate([up[:, cut:units], up[:, units + cut :]], 1)
    up_blocks = deal_over_z(
        jnp.where(low, first_half, second_half), jnp.where(low, second_half, first_half)
    )
    down = turn(down_own, stays)
    down_blocks = deal_over_z(
        jnp.where(low, down[:cut], down[cut:]), jnp.where(low, down[cut:], down[:cut])
    )
    unit_rows = jnp.concatenate([conv_weight, conv_bias[None]], 0)
    unit_rows = turn(unit_rows, stays)
    unit_rows = jnp.where(low, unit_rows[:, :cut], unit_rows[:, cut:])
    mix_own = (pool_mix * pool_mix_scale).astype(half)
    mix = jnp.where(stays, mix_own, flip(mix_own, FLIP_CORE))
    window = x * 2 + y
    scale_window = lax.dynamic_slice_in_dim(pool_in_scale, window * own_width, own_width, 0)
    mask = window_mask(window)

    values = (dot_blocks(normed, in_blocks, key) * scale_window).astype(half)
    values, *late = lax.optimization_barrier([values] + out_blocks[4:])
    out_blocks = out_blocks[:4] + late
    deviation = deviation_of(values, mask)
    pooled = dot(deviation, mix).astype(half)
    out_full = in_place(out_blocks, key, 1)
    mixer_out = None
    for j in (3, 1, 2, 0):
        partial = dot(pooled[j * rows : (j + 1) * rows], out_full).astype(half)
        if j > 0:
            partial = flip(partial, j * FLIP_X)
        partial = partial.astype(jnp.float32)
        mixer_out = partial if mixer_out is None else mixer_out + partial
    first = (plain_norm(residual_scale * stream + mixer_out) * norm1_gain + norm1_bias).astype(half)
    second = plain_norm(first.astype(jnp.float32)).astype(half)
    second_z = flip(second, FLIP_Z1)
    near = jnp.concatenate(to_plane(second), 0)
    far = to_plane(second_z)

    up_blocks[6:] = lax.optimization_barrier([near] + up_blocks[6:])[1:]
    up_pairs = [in_place(up_blocks[2 * s : 2 * s + 2], core, 0) for s in range(4)]
    near = hidden_units(near, up_pairs, z, unit_rows)
    near, *far[3:] = lax.optimization_barrier([near] + far[3:])
    far = jnp.concatenate(far, 0)
    far = hidden_units(far, up_pairs, z, unit_rows)

    blocks = [side[j * rows : (j + 1) * rows] for side in (near, far) for j in range(4)]

    def places(start, later):
        one, two = later
        return jnp.concatenate([blocks[start + k] for k in (0, two, one, one + two)], 0)

    sums = [None] * 4
    sent = [None] * 4
    for s, (one, *later) in enumerate(ORDERS):
        arranged = ORDERS[s ^ 1][1:] if one == 4 else later
        parts = [places(one, arranged), places(0, later)] + down_blocks[2 * s : 2 * s + 2]
        away, kept, *pair = lax.optimization_barrier(parts)
        columns = in_place(pair, core, 1)
        sent[s] = flip(dot(away, columns).astype(half), one * FLIP_X)
        sums[s] = (kept, columns)
    for s, (one, two, three) in enumerate(ORDERS):
        total = dot(*sums[s]) + sent[s ^ 1 if one == 4 else s].astype(jnp.float32)
        moved = flip(total[2 * rows :].astype(half), two * FLIP_X)
        sums[s] = total[: 2 * rows] + moved.astype(jnp.float32)
    for s, (_, _, three) in enumerate(ORDERS):
        sent[s] = flip(sums[s][rows:].astype(half), three * FLIP_X)
    for s, (_, _, three) in enumerate(ORDERS):
        sums[s] = sums[s][:rows] + sent[s ^ 1 if three == 4 else s].astype(jnp.float32)
    ffn_out = in_place(sums, z, 1)
    last = plain_norm(residual_scale * first.astype(jnp.float32) + ffn_out) * norm2_gain + norm2_bias
    return last.astype(half)


def solution(mesh):
    placed = (
        P(("fs", "tp"), None),
        P("fs", None),
        P(None, "tp"),
        P("tp", "fs"),
        P("fs", "tp"),
        P("fs", "tp"),
        P("tp", "fs"),
        P(None, "tp"),
        P("tp"),
        P(),
        P("tp"),
        P("fs"),
        P("tp"),
        P("tp"),
        P("fs"),
        P(),
        P(),
        P(),
        P(),
    )
    if mesh.shape["fs"] != SLOTS or mesh.shape["tp"] != 2 * CORES:
        return mapped(gathered_body, mesh, placed)

    return mapped(exchange_body, mesh, placed)


def mapped(body, mesh, placed):
    return jax.shard_map(
        body, mesh=mesh, in_specs=placed, out_specs=P(("fs", "tp"), None), check_vma=False
    )
```

```python
import jax
import jax.numpy as jnp
from jax import lax
from jax.sharding import PartitionSpec as P

GRID = 64
GROUP = 512
CORES = 2

epsilon = 1e-06
residual_scale = 2.0**0.5
window_spans = (2, 4, 8, 16)
axes = ("fs", "tp")


def plain_norm(stream):
    centre = jnp.mean(stream, -1, keepdims=True)
    spread = jnp.mean(jnp.square(stream - centre), -1, keepdims=True)
    return (stream - centre) * lax.rsqrt(spread + epsilon)


def conv_rows(gate_cells, conv_weight, conv_bias):
    padded = jnp.pad(gate_cells, ((0, 0), (1, 1), (0, 0)))
    return (
        conv_weight[0] * padded[:, :-2]
        + conv_weight[1] * gate_cells
        + conv_weight[2] * padded[:, 2:]
        + conv_bias
    )


def window_mask(window):
    half = jnp.int32(window_spans[0] // 2)
    for place, span in enumerate(window_spans):
        half = jnp.where(window == place, span // 2, half)
    rows = lax.broadcasted_iota(jnp.int32, (GRID, GRID), 0)
    columns = lax.broadcasted_iota(jnp.int32, (GRID, GRID), 1)
    inside = (columns >= rows - half) & (columns < rows + half)
    places = lax.broadcasted_iota(jnp.int32, (GRID, 1), 0)
    count = jnp.minimum(places + half, GRID) - jnp.maximum(places - half, 0)
    return inside.astype(jnp.bfloat16), count.astype(jnp.float32)


def deviation_of(values, mask):
    row_count, width = values.shape
    cells = values.reshape(row_count // GRID, GRID, width)
    inside, count = mask
    totals = jnp.einsum("pq,rqc->rpc", inside, cells, preferred_element_type=jnp.float32)
    averages = totals / count[None]
    return (averages - cells.astype(jnp.float32)).astype(jnp.bfloat16).reshape(row_count, width)


def gathered_body(
    tokens,
    pool_in,
    pool_mix,
    pool_out,
    ffn_value,
    ffn_gate,
    ffn_down,
    conv_weight,
    conv_bias,
    pool_in_scale,
    pool_mix_scale,
    pool_out_scale,
    value_scale,
    gate_scale,
    down_scale,
    norm1_gain,
    norm1_bias,
    norm2_gain,
    norm2_bias,
):
    place = lax.axis_index("tp")
    own_width = pool_mix.shape[1]
    window = place * own_width // GROUP
    window_start = window * GROUP
    window_columns = lax.dynamic_slice_in_dim(pool_in, window_start, GROUP, 1).astype(jnp.bfloat16)
    scale_window = lax.dynamic_slice_in_dim(pool_in_scale, window_start, GROUP, 0)
    out_scale = lax.all_gather(pool_out_scale, "fs", axis=0, tiled=True)
    final_scale = lax.all_gather(down_scale, "fs", axis=0, tiled=True)
    in_window = lax.all_gather(window_columns, "fs", axis=0, tiled=True)
    out_rows = lax.all_gather(pool_out.astype(jnp.bfloat16), "fs", axis=1, tiled=True)
    value_shard = ffn_value.astype(jnp.bfloat16)
    gate_shard = ffn_gate.astype(jnp.bfloat16)
    down_shard = ffn_down.astype(jnp.bfloat16)
    stream = tokens.astype(jnp.float32)
    normed = plain_norm(stream).astype(jnp.bfloat16)
    values = (
        jnp.dot(
            lax.all_gather(normed, "tp", axis=0, tiled=True),
            in_window,
            preferred_element_type=jnp.float32,
        )
        * scale_window
    ).astype(jnp.bfloat16)
    deviation = deviation_of(values, window_mask(window))
    pooled = (
        jnp.dot(deviation, pool_mix.astype(jnp.bfloat16), preferred_element_type=jnp.float32)
        * pool_mix_scale
    ).astype(jnp.bfloat16)
    mixer_partial = jnp.dot(pooled, out_rows, preferred_element_type=jnp.float32)
    mixer_out = (
        lax.psum_scatter(
            mixer_partial.astype(jnp.bfloat16), "tp", scatter_dimension=0, tiled=True
        ).astype(jnp.float32)
        * out_scale
    )
    first = (plain_norm(residual_scale * stream + mixer_out) * norm1_gain + norm1_bias).astype(
        jnp.bfloat16
    )
    normed_two = plain_norm(first.astype(jnp.float32)).astype(jnp.bfloat16)
    hidden_width = value_shard.shape[1]
    gathered = lax.all_gather(normed_two, "tp", axis=0, tiled=True)
    value_full = lax.all_gather(value_shard, "fs", axis=0, tiled=True)
    gate_full = lax.all_gather(gate_shard, "fs", axis=0, tiled=True)
    value = jnp.dot(gathered, value_full, preferred_element_type=jnp.float32) * value_scale
    gate = jnp.dot(gathered, gate_full, preferred_element_type=jnp.float32) * gate_scale
    conv = conv_rows(gate.reshape(-1, GRID, hidden_width), conv_weight, conv_bias).reshape(
        -1, hidden_width
    )
    hidden = (value * jax.nn.silu(conv)).astype(jnp.bfloat16)
    down_full = lax.all_gather(down_shard, "fs", axis=1, tiled=True)
    partial_value = jnp.dot(hidden, down_full, preferred_element_type=jnp.float32)
    summed = lax.psum_scatter(
        partial_value.astype(jnp.bfloat16), "tp", scatter_dimension=0, tiled=True
    ).astype(jnp.float32)
    ffn_out = summed * final_scale
    return (
        plain_norm(residual_scale * first.astype(jnp.float32) + ffn_out) * norm2_gain + norm2_bias
    ).astype(jnp.bfloat16)


FLIP_CORE, FLIP_X, FLIP_Y, FLIP_Z1, FLIP_Z2 = 1, 2, 4, 8, 16
SLOTS = 8


def flip(array, mask):
    return lax.ppermute(array, axes, [(device, device ^ mask) for device in range(32)])


def turn(array, stays):
    pairs = [(d, d ^ 5) for d in range(32) if ((d >> 2) & 1) != (d & 1)]
    moved = lax.ppermute(array, axes, pairs)
    return jnp.where(stays, array, moved)


def in_place(blocks, key, axis):
    size = blocks[0].shape[axis]
    shape = list(blocks[0].shape)
    shape[axis] = size * len(blocks)
    whole = jnp.zeros(shape, blocks[0].dtype)
    for k, block in enumerate(blocks):
        whole = lax.dynamic_update_slice_in_dim(whole, block, (k ^ key) * size, axis)
    return whole


def with_other_core(pieces):
    blocks = []
    for own in pieces:
        blocks += [own, flip(own, FLIP_CORE)]
    return blocks


def spread_over_z(piece):
    one = flip(piece, FLIP_Z1)
    two = flip(piece, FLIP_Z2)
    three = flip(two, FLIP_Z1)
    return with_other_core([piece, one, two, three])


def deal_over_z(even, odd):
    one = flip(odd, FLIP_Z1)
    two = flip(even, FLIP_Z2)
    three = flip(odd, FLIP_Z1 | FLIP_Z2)
    return with_other_core([even, one, two, three])


def to_plane(array):
    middle = array.shape[0] // 2
    by_x = flip(array, FLIP_X)
    by_y = flip(array, FLIP_Y)
    upper = flip(by_y[:middle], FLIP_X)
    lower = flip(by_x[middle:], FLIP_Y)
    return [array, by_x, by_y, upper, lower]


def dot(left, right):
    return jnp.dot(left, right, preferred_element_type=jnp.float32)


def dot_blocks(left, blocks, key, order=None):
    width = blocks[0].shape[0]
    total = None
    for k in order or range(len(blocks)):
        block = blocks[k]
        columns = lax.dynamic_slice_in_dim(left, (k ^ key) * width, width, 1)
        part = dot(columns, block)
        total = part if total is None else total + part
    return total


def hidden_units(left, up_pairs, z, unit_rows):
    both_sums = dot_blocks(left, up_pairs, z, (0, 1, 3, 2))
    cut = both_sums.shape[1] // 2
    value, gate = both_sums[:, :cut], both_sums[:, cut:]
    conv = conv_rows(gate.reshape(-1, GRID, cut), unit_rows[:3], unit_rows[3]).reshape(-1, cut)
    return (value * jax.nn.silu(conv)).astype(jnp.bfloat16)


ORDERS = ((1, 2, 4), (2, 1, 4), (2, 1, 4), (1, 2, 4))


def exchange_body(
    tokens,
    pool_in,
    pool_mix,
    pool_out,
    ffn_value,
    ffn_gate,
    ffn_down,
    conv_weight,
    conv_bias,
    pool_in_scale,
    pool_mix_scale,
    pool_out_scale,
    value_scale,
    gate_scale,
    down_scale,
    norm1_gain,
    norm1_bias,
    norm2_gain,
    norm2_bias,
):
    half = jnp.bfloat16
    fs, tp = lax.axis_index("fs"), lax.axis_index("tp")
    z, y, x, core = fs >> 1, fs & 1, tp >> 1, tp & 1
    key = z * 2 + core
    stays = y == core
    low = (z & 1) == 0
    rows, own_width = tokens.shape[0], pool_mix.shape[1]
    units = ffn_value.shape[1]
    cut = units // 2

    in_own = lax.dynamic_slice_in_dim(pool_in, tp * own_width, own_width, 1)
    in_piece = turn(in_own.astype(half), stays)
    out_piece = turn((pool_out * pool_out_scale).astype(half), stays)
    in_blocks = spread_over_z(in_piece)
    out_blocks = spread_over_z(out_piece)

    stream = tokens.astype(jnp.float32)
    normed_own = plain_norm(stream).astype(half)
    normed_y = flip(normed_own, FLIP_Y)
    normed = jnp.concatenate(
        [normed_own, flip(normed_own, FLIP_X), normed_y, flip(normed_y, FLIP_X)], 0
    )

    value_own = (ffn_value * value_scale).astype(half)
    gate_own = (ffn_gate * gate_scale).astype(half)
    up_own = jnp.concatenate([value_own, gate_own], 1)
    down_own = (ffn_down * down_scale).astype(half)
    up = turn(up_own, stays)
    first_half = jnp.concatenate([up[:, :cut], up[:, units : units + cut]], 1)
    second_half = jnp.concatenate([up[:, cut:units], up[:, units + cut :]], 1)
    up_blocks = deal_over_z(
        jnp.where(low, first_half, second_half), jnp.where(low, second_half, first_half)
    )
    down = turn(down_own, stays)
    down_blocks = deal_over_z(
        jnp.where(low, down[:cut], down[cut:]), jnp.where(low, down[cut:], down[:cut])
    )
    unit_rows = jnp.concatenate([conv_weight, conv_bias[None]], 0)
    unit_rows = turn(unit_rows, stays)
    unit_rows = jnp.where(low, unit_rows[:, :cut], unit_rows[:, cut:])
    mix_own = (pool_mix * pool_mix_scale).astype(half)
    mix = jnp.where(stays, mix_own, flip(mix_own, FLIP_CORE))
    window = x * 2 + y
    scale_window = lax.dynamic_slice_in_dim(pool_in_scale, window * own_width, own_width, 0)
    mask = window_mask(window)

    values = (dot_blocks(normed, in_blocks, key) * scale_window).astype(half)
    values, *late = lax.optimization_barrier([values] + out_blocks[4:])
    out_blocks = out_blocks[:4] + late
    deviation = deviation_of(values, mask)
    pooled = dot(deviation, mix).astype(half)
    out_full = in_place(out_blocks, key, 1)
    mixer_out = None
    for j in (3, 1, 2, 0):
        partial = dot(pooled[j * rows : (j + 1) * rows], out_full).astype(half)
        if j > 0:
            partial = flip(partial, j * FLIP_X)
        partial = partial.astype(jnp.float32)
        mixer_out = partial if mixer_out is None else mixer_out + partial
    first = (plain_norm(residual_scale * stream + mixer_out) * norm1_gain + norm1_bias).astype(half)
    second = plain_norm(first.astype(jnp.float32)).astype(half)
    second_z = flip(second, FLIP_Z1)
    near = jnp.concatenate(to_plane(second), 0)
    far = to_plane(second_z)

    up_blocks[4:6] = lax.optimization_barrier([near] + up_blocks[4:6])[1:]
    up_blocks[6:] = lax.optimization_barrier([near] + up_blocks[6:])[1:]
    up_pairs = [in_place(up_blocks[2 * s : 2 * s + 2], core, 0) for s in range(4)]
    near = hidden_units(near, up_pairs, z, unit_rows)
    near, *far[3:] = lax.optimization_barrier([near] + far[3:])
    far = jnp.concatenate(far, 0)
    far = hidden_units(far, up_pairs, z, unit_rows)

    blocks = [side[j * rows : (j + 1) * rows] for side in (near, far) for j in range(4)]

    def places(start, later):
        one, two = later
        return jnp.concatenate([blocks[start + k] for k in (0, two, one, one + two)], 0)

    sums = [None] * 4
    sent = [None] * 4
    for s, (one, *later) in enumerate(ORDERS):
        arranged = ORDERS[s ^ 1][1:] if one == 4 else later
        parts = [places(one, arranged), places(0, later)] + down_blocks[2 * s : 2 * s + 2]
        away, kept, *pair = lax.optimization_barrier(parts)
        columns = in_place(pair, core, 1)
        sent[s] = flip(dot(away, columns).astype(half), one * FLIP_X)
        sums[s] = (kept, columns)
    for s, (one, two, three) in enumerate(ORDERS):
        total = dot(*sums[s]) + sent[s ^ 1 if one == 4 else s].astype(jnp.float32)
        moved = flip(total[2 * rows :].astype(half), two * FLIP_X)
        sums[s] = total[: 2 * rows] + moved.astype(jnp.float32)
    for s, (_, _, three) in enumerate(ORDERS):
        sent[s] = flip(sums[s][rows:].astype(half), three * FLIP_X)
    for s, (_, _, three) in enumerate(ORDERS):
        sums[s] = sums[s][:rows] + sent[s ^ 1 if three == 4 else s].astype(jnp.float32)
    ffn_out = in_place(sums, z, 1)
    last = plain_norm(residual_scale * first.astype(jnp.float32) + ffn_out) * norm2_gain + norm2_bias
    return last.astype(half)


def solution(mesh):
    placed = (
        P(("fs", "tp"), None),
        P("fs", None),
        P(None, "tp"),
        P("tp", "fs"),
        P("fs", "tp"),
        P("fs", "tp"),
        P("tp", "fs"),
        P(None, "tp"),
        P("tp"),
        P(),
        P("tp"),
        P("fs"),
        P("tp"),
        P("tp"),
        P("fs"),
        P(),
        P(),
        P(),
        P(),
    )
    if mesh.shape["fs"] != SLOTS or mesh.shape["tp"] != 2 * CORES:
        return mapped(gathered_body, mesh, placed)

    return mapped(exchange_body, mesh, placed)


def mapped(body, mesh, placed):
    return jax.shard_map(
        body, mesh=mesh, in_specs=placed, out_specs=P(("fs", "tp"), None), check_vma=False
    )
```
